32 devices in a mesh: sp: 8 (over z, core), tp: 4 (over y, x).
Axes of the slice: x: 2, y: 2, z: 4, core: 2. Of those that a mesh axis runs over, the one named last changes fastest.
Arguments:
- cotangent: bfloat16 [1024, 2048], P('sp'), may hold values from -6 to 6
- normed: bfloat16 [1024, 2048], P('sp'), may hold values from -6 to 6
- inverse_root_mean_square: float32 [1024], P('sp'), may hold values from 0.5 to 2
- expert_norm_scale: float32 [2048], replicated, may hold values from 0.1 to 1.9
- routes: int32 [1024, 2], P('sp'), may hold values from 0 to 7, all different within a row; in each aligned block of 128 rows (0 to 127, 128 to 255, ...) at most 64 rows name the same one
- route_probability_weight: float32 [1024, 2], P('sp'), may hold values from 0.2 to 1
- gate_weight: bfloat16 [8, 2048, 2048], P('sp', None, 'tp'), may hold values from -0.125 to 0.125
- up_weight: bfloat16 [8, 2048, 2048], P('sp', None, 'tp'), may hold values from -0.125 to 0.125
- down_weight: bfloat16 [8, 2048, 2048], P('sp', 'tp'), may hold values from -0.125 to 0.125
- recurrence_input: bfloat16 [1024, 1024], P('sp', 'tp'), may hold values from -6 to 6
- recurrence_gate_logits: bfloat16 [1024, 1024], P('sp', 'tp'), may hold values from -6 to 6
- input_gate_logits: bfloat16 [1024, 1024], P('sp', 'tp'), may hold values from -6 to 6
- channel_decay_weight: float32 [1024], P('tp'), may hold values from 3 to 20
- extra_log_decay: float32 [1024, 1024], P('sp', 'tp'), may hold values from -1 to 0
- output_matrix: bfloat16 [2048, 1024], P(None, 'tp'), may hold values from -0.1875 to 0.1875
Outputs:
- grad_gate: bfloat16 [8, 2048, 2048], P('sp', None, 'tp')
- grad_up: bfloat16 [8, 2048, 2048], P('sp', None, 'tp')
- grad_down: bfloat16 [8, 2048, 2048], P('sp', 'tp')
- grad_out_weight: float32 [2048, 1024], P('sp', 'tp')
- grad_rec_input: float32 [1024, 1024], P('sp', 'tp')
- grad_decay_gate: float32 [1024, 1024], P('sp', 'tp')
- grad_input_gate: float32 [1024, 1024], P('sp', 'tp')
The draws below stay inside these ranges and needn't reach their ends.
Inputs may be any that keep to these rules, and one draw needn't show every extreme that they name: `routes`: each row names 2 different experts; among the rows of one device no expert is named more than 64 times.
All inputs are finite; a program needn't handle non-finite values.
Results may differ from the reference program's by a relative error of at most 0.025.
Values may be sent and summed in bfloat16 or wider, within the bound.
No kernel may reach another device: no remote copies, remote signals or barrier semaphores. Data moves between devices by JAX's collectives and lax.ppermute only.
A program may use at most 64 MiB of HBM per device.

```python
import math
import jax
import jax.numpy as jnp
import numpy as np
from jax import lax

D = 2048
C = 1024
FF = 2048
TOPK = 2
TOK_DEV = 128
EXPERTS = 8
CAP = 64
TOKENS = 1024
N_SP = 8
N_TP = 4


def draw_channel_decay_weight(key, part):
    first, second, third = jax.random.split(key, 3)
    share = 0.5
    quick = jax.random.uniform(first, (C,), jnp.float32) < share
    slow_rate = jnp.exp(jax.random.uniform(second, (C,), jnp.float32, jnp.log(0.02), jnp.log(0.12))) / TOKENS
    quick_rate = jnp.exp(jax.random.uniform(third, (C,), jnp.float32, jnp.log(0.005), jnp.log(0.02)))
    rate = jnp.where(quick, quick_rate, slow_rate)
    return (-jnp.log(jnp.expm1(rate))).astype(jnp.float32)


def draw_extra_log_decay(key, part):
    first, second = jax.random.split(key, 2)
    places = jax.random.randint(first, (3,), 0, TOKENS)
    struck = jnp.any(jnp.arange(TOKENS)[:, None] == places[None, :], axis=1)
    depth = jnp.log(jax.random.uniform(second, (TOKENS, C), jnp.float32, 0.65, 0.85))
    return jnp.where(struck[:, None], depth, 0.0).astype(jnp.float32)


def draw_recurrence_gate_logits(key, part):
    first, second = jax.random.split(key, 2)
    blocks = TOKENS // TOK_DEV
    offset = jax.random.uniform(first, (blocks,), jnp.float32, -1.0, 1.0)
    noise = jnp.clip(jax.random.normal(second, (TOKENS, C), jnp.float32) * 0.7, -3.5, 3.5)
    return (noise + jnp.repeat(offset, TOK_DEV)[:, None]).astype(jnp.bfloat16)


def raised(drawn, own_key, source, target, shards_of, factor):
    owner, partner = [(jnp.arange(drawn.shape[position]) // (drawn.shape[position] // shards_of)).reshape([-1 if axis == position else 1 for axis in range(drawn.ndim)]) for position in (source, target)]
    chosen = jax.random.permutation(own_key, shards_of)[partner]
    strong = (owner == chosen) | (owner == (partner + shards_of // 2) % shards_of)
    return jnp.where(strong, factor * drawn, drawn)


def shard_levels(stream_key, extent, cuts, least, largest):
    factor_of, own = 1.0, jax.random.fold_in(stream_key, 6)
    for axis_at, parts in cuts:
        draws = jnp.exp(jax.random.uniform(jax.random.fold_in(own, axis_at), (parts,), jnp.float32, least / len(cuts), largest / len(cuts)))
        factor_of = factor_of * jnp.repeat(draws, extent[axis_at] // parts).reshape([-1 if axis == axis_at else 1 for axis in range(len(extent))])
    return factor_of


def routed_block(key, own, number, rows, number_of, top, most, lean):
    order = jax.random.permutation(key, number_of)
    packed, ordinary = shares(number_of, rows * top, most, lean, True), shares(number_of, rows * top, most, lean, False)
    places = jnp.arange(number_of)

    def named(tallies, rotation):
        used = int((tallies > 0).sum())
        fixed = max(1, used // 4)
        moved = fixed + (places - fixed + rotation * (used - fixed)) % max(1, number_of - fixed)
        return jnp.zeros((number_of,), jnp.int32).at[order[jnp.where(places < fixed, places, moved)]].set(jnp.asarray(tallies, jnp.int32))

    tallies = jnp.where(number % 4 == 0, named(packed, number // 4), named(ordinary, number - number // 4 - 1))
    mixed = jax.random.permutation(jax.random.fold_in(own, 3), number_of)
    source_of, receiver = mixed[0:number_of // 2 * 2:2], mixed[1:number_of // 2 * 2:2]
    room = jnp.minimum(tallies[source_of] - 1, most - tallies[receiver]) // 2
    room = jnp.where((source_of == order[0]) | (receiver == order[0]) | (tallies[receiver] == 0), 0, jnp.maximum(room, 0))
    moved = jax.random.randint(jax.random.fold_in(own, 4), (number_of // 2,), 0, 1 << 20) % (room + 1)
    tallies = tallies.at[source_of].add(-moved).at[receiver].add(moved)
    items = jnp.searchsorted(jnp.cumsum(tallies), jnp.arange(rows * top), side="right").astype(jnp.int32)
    listing = items.reshape(top, rows).T
    listing = listing[jax.random.permutation(jax.random.fold_in(own, 1), rows)]
    rotation = jax.random.randint(jax.random.fold_in(own, 2), (rows, 1), 0, top)
    return jnp.take_along_axis(listing, (jnp.arange(top)[None, :] + rotation) % top, axis=1)


def shares(amount, total, most, lean, full):
    loads = [(1 << 20) // math.isqrt(grade ** lean) + 1 for grade in range(1, amount + 1)]
    largest = most if full else min(most, max(-(-total // amount), total * loads[0] // sum(loads)))
    least = 1 if total - largest >= amount - 1 else 0
    holding, rest = [largest] + [least] * (amount - 1), total - largest - least * (amount - 1)
    while rest > 0:
        candidates = [i for i in range(1, amount) if holding[i] < largest] or [i for i in range(1, amount) if holding[i] < most]
        pool, remaining = sum([loads[i] for i in candidates]), rest
        for i in candidates:
            addition = min(most - holding[i], max(1, remaining * loads[i] // pool), rest)
            holding[i] = holding[i] + addition
            rest = rest - addition
    return np.array(holding)


def gaussian(rng, shape, width, reach, cuts=(), kind=jnp.bfloat16):
    loudness = shard_levels(rng, shape, cuts, -0.22, 0.18) if cuts else 1.0
    values = jax.random.normal(rng, shape, jnp.float32) * width * loudness
    return jnp.minimum(jnp.maximum(values, -reach), reach).astype(kind)


def gaussian_with(own_key, extent, scale, bound, shards, heavy, kind=jnp.bfloat16):
    entries = scale * jax.random.normal(own_key, extent, jnp.float32)
    if shards:
        entries = entries * shard_levels(own_key, extent, shards, -0.22, 0.18)
    return jnp.clip(raised(entries, jax.random.fold_in(own_key, 3), *heavy), -bound, bound).astype(kind)


def setup_inputs(seed: int = 0) -> dict:
    key_list = jax.random.split(jax.random.key(seed), 16)
    cotangent = gaussian_with(key_list[0], (TOKENS, D), 1.0, 6.0, ((0, 8),), (0, 1, 8, 2.0))
    normed = gaussian(key_list[1], (TOKENS, D), 1.0, 6.0, ((0, 8),))
    inverse_root_mean_square = jnp.clip(jnp.exp(math.log(2.0) - 1.3862944 * jax.random.uniform(key_list[2], (TOKENS,), jnp.float32) ** shard_levels(key_list[2], (TOKENS,), ((0, 8),), -0.2, 0.2)), 0.5, 2.0)
    expert_norm_scale = jnp.clip(1.0 + 0.18 * jax.random.normal(key_list[3], (D,), jnp.float32), 0.1, 1.9)
    routes_keys = jax.random.split(jax.random.fold_in(key_list[4], 1), TOKENS // TOK_DEV)
    routes_turns = jax.random.permutation(jax.random.fold_in(key_list[4], 3), TOKENS // TOK_DEV)
    routes = jax.vmap(lambda own, number: routed_block(jax.random.fold_in(key_list[4], 2), own, number, TOK_DEV, EXPERTS, TOPK, CAP, 1))(routes_keys, routes_turns).reshape((TOKENS, TOPK))
    route_probability_weight = jnp.clip(0.2 + 0.8 * jax.random.uniform(key_list[5], (TOKENS, TOPK), jnp.float32) ** shard_levels(key_list[5], (TOKENS, TOPK), ((0, 8),), -0.2, 0.2), 0.2, 1.0)
    gate_weight = gaussian(key_list[6], (EXPERTS, D, FF), D ** -0.5, 0.125, ((0, 8), (2, 4)))
    up_weight = gaussian(key_list[7], (EXPERTS, D, FF), D ** -0.5, 0.125, ((0, 8), (2, 4)))
    down_weight = gaussian(key_list[8], (EXPERTS, FF, D), FF ** -0.5, 0.125, ((0, 8), (1, 4)))
    recurrence_input = gaussian(key_list[9], (TOKENS, C), 1.0, 6.0, ((0, 8), (1, 4)))
    recurrence_gate_logits = draw_recurrence_gate_logits(jax.random.fold_in(key_list[15], 71), 0)
    input_gate_logits = gaussian(key_list[11], (TOKENS, C), 1.0, 6.0, ((0, 8), (1, 4)))
    channel_decay_weight = draw_channel_decay_weight(jax.random.fold_in(key_list[15], 71), 0)
    extra_log_decay = draw_extra_log_decay(jax.random.fold_in(key_list[15], 71), 0)
    output_matrix = gaussian(key_list[14], (D, C), C ** -0.5, 0.1875, ((1, 4),))
    return dict(cotangent=cotangent, normed=normed, inverse_root_mean_square=inverse_root_mean_square, expert_norm_scale=expert_norm_scale, routes=routes, route_probability_weight=route_probability_weight, gate_weight=gate_weight, up_weight=up_weight, down_weight=down_weight, recurrence_input=recurrence_input, recurrence_gate_logits=recurrence_gate_logits, input_gate_logits=input_gate_logits, channel_decay_weight=channel_decay_weight, extra_log_decay=extra_log_decay, output_matrix=output_matrix)


def link(earlier, later):
    return (earlier[0] * later[0], later[0] * earlier[1] + later[1])

def expert_step(items):
    grad_in, tokens_in, gate_w, up_w, down_w = items
    rows = tokens_in.shape[0]
    gate_pre = jnp.dot(tokens_in, gate_w, preferred_element_type=jnp.float32)
    up_pre = jnp.dot(tokens_in, up_w, preferred_element_type=jnp.float32)
    sigma = jax.nn.sigmoid(gate_pre)
    swish = gate_pre * sigma
    active = (swish * up_pre).astype(jnp.bfloat16)
    d_active = jnp.dot(grad_in, down_w.T, preferred_element_type=jnp.float32)
    d_gate = (d_active * up_pre * sigma * (1.0 + gate_pre * (1.0 - sigma))).astype(jnp.bfloat16)
    d_up = (d_active * swish).astype(jnp.bfloat16)
    grad_down = jnp.dot(active.T, grad_in, preferred_element_type=jnp.float32).astype(jnp.bfloat16)
    grad_gate = jnp.dot(tokens_in.T, d_gate, preferred_element_type=jnp.float32).astype(jnp.bfloat16)
    grad_up = jnp.dot(tokens_in.T, d_up, preferred_element_type=jnp.float32).astype(jnp.bfloat16)
    block = FF // N_TP
    d_gate4 = d_gate.astype(jnp.float32).reshape(rows, N_TP, block)
    d_up4 = d_up.astype(jnp.float32).reshape(rows, N_TP, block)
    gate4 = gate_w.astype(jnp.float32).reshape(D, N_TP, block)
    up4 = up_w.astype(jnp.float32).reshape(D, N_TP, block)
    pieces = jnp.einsum('rjf,djf->jrd', d_gate4, gate4) + jnp.einsum('rjf,djf->jrd', d_up4, up4)
    rounded = lax.optimization_barrier(pieces.astype(jnp.bfloat16)).astype(jnp.float32)
    returned = lax.optimization_barrier(jnp.sum(rounded, axis=0)).astype(jnp.bfloat16)
    return (grad_gate, grad_up, grad_down, returned)

def reference(cotangent, normed, inverse_root_mean_square, expert_norm_scale, routes, route_probability_weight, gate_weight, up_weight, down_weight, recurrence_input, recurrence_gate_logits, input_gate_logits, channel_decay_weight, extra_log_decay, output_matrix):
    per_block = TOK_DEV * TOPK
    chosen = routes.reshape(N_SP, per_block)
    member = (chosen[:, :, None] == jnp.arange(EXPERTS, dtype=jnp.int32)[None, None, :]).astype(jnp.int32)
    ranking = lax.optimization_barrier(jnp.sum((jnp.cumsum(member, axis=1) - member) * member, axis=2))
    source = jnp.arange(N_SP, dtype=jnp.int32)[:, None]
    landing = (chosen * (N_SP * CAP) + source * CAP + ranking).reshape(-1).astype(jnp.int32)
    scaled = (route_probability_weight[:, :, None] * cotangent[:, None, :].astype(jnp.float32)).astype(jnp.bfloat16)
    scaled = scaled.reshape(TOKENS * TOPK, D)
    copies = jnp.repeat(normed, TOPK, axis=0)
    buffer_rows = EXPERTS * N_SP * CAP
    grad_in = jnp.zeros((buffer_rows, D), jnp.bfloat16).at[landing].set(scaled).reshape(EXPERTS, N_SP * CAP, D)
    tokens_in = jnp.zeros((buffer_rows, D), jnp.bfloat16).at[landing].set(copies).reshape(EXPERTS, N_SP * CAP, D)
    grad_gate, grad_up, grad_down, returned = lax.map(expert_step, (grad_in, tokens_in, gate_weight, up_weight, down_weight))
    back_rows = returned.reshape(buffer_rows, D)[landing]
    d_norm = lax.optimization_barrier(jnp.sum(back_rows.astype(jnp.float32).reshape(TOKENS, TOPK, D), axis=1))
    nhat = normed.astype(jnp.float32) / expert_norm_scale[None, :]
    gained = expert_norm_scale[None, :] * d_norm
    stat = lax.optimization_barrier(jnp.mean(gained * nhat, axis=1, keepdims=True))
    d_mix = (cotangent.astype(jnp.float32) + inverse_root_mean_square[:, None] * (gained - nhat * stat)).astype(jnp.bfloat16)
    retention_factor = jax.nn.sigmoid(recurrence_gate_logits.astype(jnp.float32))
    admit = jax.nn.sigmoid(input_gate_logits.astype(jnp.float32))
    signal = recurrence_input.astype(jnp.float32)
    decay_speed = jax.nn.softplus(-channel_decay_weight)
    log_retention = -8.0 * retention_factor * decay_speed[None, :] + extra_log_decay
    keep = jnp.exp(log_retention)
    scale_in = jnp.sqrt(-jnp.expm1(2.0 * log_retention))
    driven = scale_in * admit * signal
    _, state = lax.associative_scan(link, (keep, driven), axis=0)
    hidden = state.astype(jnp.bfloat16)
    state_prev = jnp.concatenate([jnp.zeros((1, C), jnp.float32), state[:-1]], axis=0)
    grad_out_weight = jnp.dot(d_mix.T, hidden, preferred_element_type=jnp.float32)
    d_state = jnp.dot(d_mix, output_matrix, preferred_element_type=jnp.float32)
    keep_next = jnp.concatenate([keep[1:], jnp.ones((1, C), jnp.float32)], axis=0)
    _, total = lax.associative_scan(link, (keep_next, d_state), reverse=True, axis=0)
    grad_rec_input = total * scale_in * admit
    grad_input_gate = total * scale_in * signal * admit * (1.0 - admit)
    d_log = total * state_prev * keep - total * admit * signal * keep * keep / scale_in
    grad_decay_gate = d_log * (-8.0 * decay_speed[None, :]) * retention_factor * (1.0 - retention_factor)
    return (grad_gate, grad_up, grad_down, grad_out_weight, grad_rec_input, grad_decay_gate, grad_input_gate)
```

```python
import functools

import jax
import jax.numpy as jnp
from jax import lax
from jax.experimental import pallas as pl
from jax.experimental.pallas import tpu as pltpu
from jax.sharding import PartitionSpec as P


F32, BF16 = jnp.float32, jnp.bfloat16
ROWS = (((0,), (0,)), ((), ()))
COLS = (((1,), (1,)), ((), ()))
PLAIN = (((1,), (0,)), ((), ()))


def dot(a, b, dims=PLAIN):
    return lax.dot_general(a, b, dims, preferred_element_type=F32)


def call(body, outs, *args, scalars=None, name=None):
    vm = pl.BlockSpec(memory_space=pltpu.VMEM)
    sm = pl.BlockSpec(memory_space=pltpu.SMEM)
    ins = ([sm] if scalars is not None else []) + [vm] * len(args)
    if scalars is not None:
        args = (scalars,) + tuple(args)
    return pl.pallas_call(
        body, out_shape=outs, in_specs=ins, out_specs=jax.tree.map(lambda _: vm, outs), name=name
    )(*args)


def swap(x, axis, m):
    n = lax.axis_size(axis)
    return lax.ppermute(x, axis, [(i, i ^ m) for i in range(n)])


def wide(t, width):
    return pl.ds(pl.multiple_of(t * width, width), width)


def pack_body(groups, tps, cap, place_ref, routes_ref, weight_ref, normed_ref, cot_ref, *outs):
    xs, ys = outs[: groups - 2], outs[groups - 2 : 2 * (groups - 2)]
    own_ref, pair_ref = outs[2 * (groups - 2) :]
    s, t = place_ref[0], place_ref[1]
    tok = normed_ref.shape[0]
    wq = normed_ref.shape[1] // tps
    e0, e1 = routes_ref[0:1, :], routes_ref[1:2, :]
    ids = lax.broadcasted_iota(jnp.int32, (groups, tok), 0)
    hit0, hit1 = ids == e0, ids == e1
    member = jnp.where(hit0 | hit1, 1.0, 0.0).astype(BF16)
    upper = (
        lax.broadcasted_iota(jnp.int32, (tok, tok), 0)
        < lax.broadcasted_iota(jnp.int32, (tok, tok), 1)
    )
    rank = dot(member, jnp.where(upper, 1.0, 0.0).astype(BF16))
    r0 = jnp.sum(jnp.where(hit0, rank, 0.0), axis=0, keepdims=True).astype(jnp.int32)
    r1 = jnp.sum(jnp.where(hit1, rank, 0.0), axis=0, keepdims=True).astype(jnp.int32)
    land0 = (e0 ^ s) * cap + r0
    land1 = (e1 ^ s) * cap + r1
    slots = lax.broadcasted_iota(jnp.int32, (groups * cap, tok), 0)
    in0, in1 = slots == land0, slots == land1
    pick = jnp.where(in0 | in1, 1.0, 0.0).astype(BF16)
    scale = jnp.sum(
        jnp.where(in0, weight_ref[0:1, :], 0.0) + jnp.where(in1, weight_ref[1:2, :], 0.0),
        axis=1,
        keepdims=True,
    )
    cols = wide(t, wq)
    far = pick[2 * cap :, :]
    xq = dot(far, normed_ref[:, cols]).astype(BF16)
    yq = (dot(far, cot_ref[:, cols]) * scale[2 * cap :, :]).astype(BF16)
    for m in range(groups - 2):
        xs[m][...] = xq[m * cap : (m + 1) * cap, :]
        ys[m][...] = yq[m * cap : (m + 1) * cap, :]
    near = pick[: 2 * cap, :]
    xn = dot(near, normed_ref[...]).astype(BF16)
    yn = (dot(near, cot_ref[...]) * scale[: 2 * cap, :]).astype(BF16)
    own_ref[:cap, :] = xn[:cap, :]
    own_ref[cap:, :] = yn[:cap, :]
    pair_ref[:cap, :] = xn[cap:, :]
    pair_ref[cap:, :] = yn[cap:, :]


def slots_body(groups, cap, place_ref, routes_ref, out_ref):
    s = place_ref[0]
    tok = routes_ref.shape[0]
    e0, e1 = routes_ref[:, 0:1], routes_ref[:, 1:2]
    ids = lax.broadcasted_iota(jnp.int32, (tok, groups), 1)
    hit0, hit1 = ids == e0, ids == e1
    member = jnp.where(hit0 | hit1, 1.0, 0.0).astype(BF16)
    lower = (
        lax.broadcasted_iota(jnp.int32, (tok, tok), 0)
        > lax.broadcasted_iota(jnp.int32, (tok, tok), 1)
    )
    rank = dot(jnp.where(lower, 1.0, 0.0).astype(BF16), member)
    r0 = jnp.sum(jnp.where(hit0, rank, 0.0), axis=1, keepdims=True).astype(jnp.int32)
    r1 = jnp.sum(jnp.where(hit1, rank, 0.0), axis=1, keepdims=True).astype(jnp.int32)
    slots = lax.broadcasted_iota(jnp.int32, (tok, groups * cap), 1)
    hit = (slots == (e0 ^ s) * cap + r0) | (slots == (e1 ^ s) * cap + r1)
    out_ref[...] = jnp.where(hit, 1.0, 0.0).astype(BF16)


def shifted(x, by, fill, down):
    pad = jnp.full((by, x.shape[1]), fill, x.dtype)
    return (
        jnp.concatenate([pad, x[:-by, :]], axis=0)
        if down
        else jnp.concatenate([x[by:, :], pad], axis=0)
    )


def scan(keep, value, forward):
    by = 1
    while by < keep.shape[0]:
        value = keep * shifted(value, by, 0.0, forward) + value
        keep = keep * shifted(keep, by, 1.0, forward)
        by *= 2
    return keep, value


def forward_body(keep_ref, driven_ref, cum_ref, state_ref, tail_ref, edge_ref):
    keep = keep_ref[...]
    cum, state = scan(keep, driven_ref[...], True)
    tail = shifted(keep, 1, 1.0, False)
    by = 1
    while by < keep.shape[0]:
        tail = tail * shifted(tail, by, 1.0, False)
        by *= 2
    cum_ref[...] = cum
    state_ref[...] = state
    tail_ref[...] = tail
    edge_ref[...] = jnp.concatenate(
        [cum[-1:, :], state[-1:, :], keep[:1, :] * tail[:1, :], jnp.zeros((5, cum.shape[1]), F32)],
        axis=0,
    )


def enter_body(groups, place_ref, cum_ref, state_ref, k1_ref, k2_ref, *rest):
    edges, (hidden_ref, kk_ref, coef_ref) = rest[:groups], rest[groups:]
    s = place_ref[0]

    def edge(i, row):
        out = edges[0][row : row + 1, :]
        for m in range(1, groups):
            out = jnp.where((s ^ m) == i, edges[m][row : row + 1, :], out)
        return out

    state_in = jnp.zeros((1, cum_ref.shape[1]), F32)
    product = jnp.ones((1, cum_ref.shape[1]), F32)
    coefs = []
    for i in range(groups):
        state_in = jnp.where(i < s, state_in * edge(i, 0) + edge(i, 1), state_in)
        coefs.append(jnp.where(i > s, product, 0.0))
        product = jnp.where(i > s, product * edge(i, 2), product)
    state = state_ref[...] + cum_ref[...] * state_in
    hidden_ref[...] = state.astype(BF16)
    before = jnp.concatenate([state_in, state[:-1, :]], axis=0)
    kk_ref[...] = before * k1_ref[...] + k2_ref[...]
    coef_ref[...] = jnp.concatenate(coefs, axis=0)


def gather_rows(cap, tps, t, first, out_ref, own_ref, pair_ref, chunks):
    out_ref[0:cap, :] = own_ref[first : first + cap, :]
    out_ref[cap : 2 * cap, :] = pair_ref[first : first + cap, :]
    base = 2 * cap
    for pieces in chunks:
        rows, width = pieces[0].shape
        for j in range(tps):
            out_ref[base : base + rows, wide(t ^ j, width)] = pieces[j][...]
        base += rows


def split(refs, tps):
    return [refs[i : i + tps] for i in range(0, len(refs), tps)]


def hidden_body(cap, tps, place_ref, gate_ref, up_ref, own_ref, pair_ref, *rest):
    pieces, (act_ref, swish_ref, slope_ref, x_ref) = rest[:-4], rest[-4:]
    gather_rows(cap, tps, place_ref[1], 0, x_ref, own_ref, pair_ref, split(pieces, tps))
    x = x_ref[...]
    gate = dot(x, gate_ref[...])
    up = dot(x, up_ref[...])
    sigma = jax.nn.sigmoid(gate)
    swish = gate * sigma
    act_ref[...] = (swish * up).astype(BF16)
    swish_ref[...] = swish
    slope_ref[...] = up * sigma * (1.0 + gate * (1.0 - sigma))


def back_body(cap, tps, place_ref, down_ref, swish_ref, slope_ref, own_ref, pair_ref, *rest):
    pieces, (dg_ref, du_ref, y_ref) = rest[:-3], rest[-3:]
    gather_rows(cap, tps, place_ref[1], cap, y_ref, own_ref, pair_ref, split(pieces, tps))
    d_act = dot(y_ref[...], down_ref[...], COLS)
    dg_ref[...] = (d_act * slope_ref[...]).astype(BF16)
    du_ref[...] = (d_act * swish_ref[...]).astype(BF16)


def part_body(tps, place_ref, gate_ref, up_ref, dg_ref, du_ref, *outs):
    t = place_ref[1]
    width = gate_ref.shape[0] // tps
    rows = outs[0].shape[0]
    dg, du = dg_ref[...], du_ref[...]
    halves = dg.shape[0] // rows
    for j in list(range(1, tps)) + [0]:
        at = wide(t ^ j, width)
        part = dot(dg, gate_ref[at, :], COLS) + dot(du, up_ref[at, :], COLS)
        for h in range(halves):
            outs[h * tps + j][...] = part[h * rows : (h + 1) * rows, :].astype(BF16)


def grads_body(act_ref, dg_ref, du_ref, x_ref, y_ref, gg_ref, gu_ref, gd_ref):
    x = x_ref[...]
    gg_ref[...] = dot(x, dg_ref[...], ROWS).astype(BF16)
    gu_ref[...] = dot(x, du_ref[...], ROWS).astype(BF16)
    gd_ref[...] = dot(act_ref[...], y_ref[...], ROWS).astype(BF16)


def sums_body(cap, *refs):
    tps = len(refs) // 1
    pieces, outs = refs[: -(refs[0].shape[0] // cap)], refs[-(refs[0].shape[0] // cap) :]
    total = pieces[0][...].astype(F32)
    for p in pieces[1:]:
        total = total + p[...].astype(F32)
    for m, o in enumerate(outs):
        o[...] = total[m * cap : (m + 1) * cap, :].astype(BF16)


def combine_body(slots_ref, *rest):
    blocks, out_ref = rest[:-1], rest[-1]
    rows = jnp.concatenate([b[...] for b in blocks], axis=0)
    out_ref[...] = dot(slots_ref[...], rows).astype(BF16)


def mix_body(tps, groups, place_ref, inv_ref, gain_ref, normed_ref, cot_ref, mat_ref, keep_ref, *rest):
    pieces, (mix_ref, grad_ref, edge_ref, dn_ref) = rest[:tps], rest[tps:]
    t = place_ref[1]
    for j in range(tps):
        dn_ref[:, wide(t ^ j, pieces[j].shape[1])] = pieces[j][...]
    dn = dn_ref[...].astype(F32)
    normed = normed_ref[...].astype(F32)
    gain = gain_ref[...]
    stat = jnp.sum(dn * normed, axis=1, keepdims=True) * (1.0 / dn.shape[1])
    mix = cot_ref[...].astype(F32) + inv_ref[...] * (gain * dn - (normed / gain) * stat)
    mix = mix.astype(BF16)
    mix_ref[...] = mix
    keep = keep_ref[...]
    d_state = dot(mix, mat_ref[...])
    _, grad = scan(shifted(keep, 1, 1.0, False), d_state, False)
    grad_ref[...] = grad
    edge_ref[...] = keep[:1, :] * grad[:1, :]


def sds(shape, dtype):
    return jax.ShapeDtypeStruct(shape, dtype)


def shards(
    cotangent,
    normed,
    inverse_root_mean_square,
    expert_norm_scale,
    routes,
    route_probability_weight,
    gate_weight,
    up_weight,
    down_weight,
    recurrence_input,
    recurrence_gate_logits,
    input_gate_logits,
    channel_decay_weight,
    extra_log_decay,
    output_matrix,
):
    tok, features = normed.shape
    groups, tps = lax.axis_size("sp"), lax.axis_size("tp")
    cap = 2 * routes.shape[1] * tok // groups
    rows = groups * cap
    width = features // tps
    s, t = lax.axis_index("sp"), lax.axis_index("tp")
    place = jnp.stack([s, t]).astype(jnp.int32)
    gate_w, up_w, down_w = gate_weight[0], up_weight[0], down_weight[0]
    hid = gate_w.shape[1]
    chan = output_matrix.shape[1]

    block = sds((cap, width), BF16)
    both = sds((2 * cap, features), BF16)
    packed = call(
        functools.partial(pack_body, groups, tps, cap),
        [block] * (2 * (groups - 2)) + [both, both],
        routes.T,
        route_probability_weight.T,
        normed,
        cotangent,
        scalars=place,
        name="pack",
    )
    xs, ys = packed[: groups - 2], packed[groups - 2 : 2 * (groups - 2)]
    own, pair = packed[-2], packed[-1]
    pair = swap(pair, "sp", 1)

    def spread(blocks):
        mine = [swap(b, "sp", m + 2) for m, b in enumerate(blocks)]
        mine = jnp.concatenate(mine, axis=0)
        return [mine] + [swap(mine, "tp", j) for j in range(1, tps)]

    xp = spread(xs)
    yp = spread(ys)

    retain = jax.nn.sigmoid(recurrence_gate_logits.astype(F32))
    admit = jax.nn.sigmoid(input_gate_logits.astype(F32))
    signal = recurrence_input.astype(F32)
    speed = -8.0 * jax.nn.softplus(-channel_decay_weight)[None, :]
    log_keep = retain * speed + extra_log_decay
    keep = jnp.exp(log_keep)
    scale_in = jnp.sqrt(-jnp.expm1(2.0 * log_keep))
    opened = scale_in * admit
    driven = opened * signal
    slope = driven * (1.0 - admit)
    decay = speed * retain * (1.0 - retain)
    k1 = keep * decay
    k2 = -admit * signal * keep * keep / scale_in * decay
    plane = sds((tok, chan), F32)
    cum, state_loc, tail, edge = call(
        forward_body, [plane, plane, plane, sds((8, chan), F32)], keep, driven, name="local_scan"
    )
    edges = [edge] + [swap(edge, "sp", m) for m in range(1, groups)]
    hidden, kk, coef = call(
        functools.partial(enter_body, groups),
        [sds((tok, chan), BF16), plane, sds((groups, chan), F32)],
        cum,
        state_loc,
        k1,
        k2,
        *edges,
        scalars=place,
        name="enter",
    )
    slots = call(
        functools.partial(slots_body, groups, cap),
        sds((tok, rows), BF16),
        routes,
        scalars=place,
        name="slots",
    )
    hiddens = [hidden] + [swap(hidden, "sp", m) for m in range(1, groups)]

    wide_rows = sds((rows, hid), F32)
    thin_rows = sds((rows, hid), BF16)
    full_rows = sds((rows, features), BF16)
    act, swish, bend, x_all = call(
        functools.partial(hidden_body, cap, tps),
        [thin_rows, wide_rows, wide_rows, full_rows],
        gate_w,
        up_w,
        own,
        pair,
        *xp,
        scalars=place,
        name="hidden",
    )
    d_gate, d_up, y_all = call(
        functools.partial(back_body, cap, tps),
        [thin_rows, thin_rows, full_rows],
        down_w,
        swish,
        bend,
        own,
        pair,
        *yp,
        scalars=place,
        name="back",
    )
    halves = 2
    parts = call(
        functools.partial(part_body, tps),
        [sds((rows // halves, width), BF16)] * (halves * tps),
        gate_w,
        up_w,
        d_gate,
        d_up,
        scalars=place,
        name="part",
    )
    per = groups // halves
    blocks = [None] * groups
    for h in reversed(range(halves)):
        mine = parts[h * tps : (h + 1) * tps]
        got = [mine[0]] + [swap(mine[j], "tp", j) for j in range(1, tps)]
        summed = call(
            functools.partial(sums_body, cap), [block] * per, *got, name=f"sums{h}"
        )
        for i in reversed(range(per)):
            m = h * per + i
            blocks[m] = swap(summed[i], "sp", m) if m else summed[i]

    grad_gate, grad_up, grad_down = call(
        grads_body,
        [sds((features, hid), BF16), sds((features, hid), BF16), sds((hid, features), BF16)],
        act,
        d_gate,
        d_up,
        x_all,
        y_all,
        name="grads",
    )

    d_norm = call(combine_body, sds((tok, width), BF16), slots, *blocks, name="combine")
    norms = [d_norm] + [swap(d_norm, "tp", j) for j in range(1, tps)]
    d_mix, grad_loc, late, _ = call(
        functools.partial(mix_body, tps, groups),
        [sds((tok, features), BF16), plane, sds((1, chan), F32), sds((tok, features), BF16)],
        inverse_root_mean_square[:, None],
        expert_norm_scale[None, :],
        normed,
        cotangent,
        output_matrix,
        keep,
        *norms,
        scalars=place,
        name="mix",
    )
    strip = features // groups
    mixes = [
        lax.dynamic_slice_in_dim(d_mix, (s ^ m) * strip, strip, 1) for m in range(groups)
    ]
    mixes = [mixes[0]] + [swap(mixes[m], "sp", m) for m in range(1, groups)]
    grad_out_weight = dot(
        jnp.concatenate(mixes, axis=0), jnp.concatenate(hiddens, axis=0), ROWS
    )
    lates = lax.all_gather(late, "sp", axis=0, tiled=True)
    enter = jnp.sum(coef * lates, axis=0, keepdims=True)
    total = grad_loc + tail * enter
    return (
        grad_gate[None],
        grad_up[None],
        grad_down[None],
        grad_out_weight,
        total * opened,
        total * kk,
        total * slope,
    )


def solution(mesh):
    return jax.shard_map(
        shards,
        mesh=mesh,
        in_specs=(
            P("sp", None),
            P("sp", None),
            P("sp"),
            P(),
            P("sp", None),
            P("sp", None),
            P("sp", None, "tp"),
            P("sp", None, "tp"),
            P("sp", "tp", None),
            P("sp", "tp"),
            P("sp", "tp"),
            P("sp", "tp"),
            P("tp"),
            P("sp", "tp"),
            P(None, "tp"),
        ),
        out_specs=(
            P("sp", None, "tp"),
            P("sp", None, "tp"),
            P("sp", "tp", None),
            P("sp", "tp"),
            P("sp", "tp"),
            P("sp", "tp"),
            P("sp", "tp"),
        ),
        check_vma=False,
    )
```

```python
import functools

import jax
import jax.numpy as jnp
from jax import lax
from jax.experimental import pallas as pl
from jax.experimental.pallas import tpu as pltpu
from jax.sharding import PartitionSpec as P


F32, BF16 = jnp.float32, jnp.bfloat16
ROWS = (((0,), (0,)), ((), ()))
COLS = (((1,), (1,)), ((), ()))
PLAIN = (((1,), (0,)), ((), ()))


def dot(a, b, dims=PLAIN):
    return lax.dot_general(a, b, dims, preferred_element_type=F32)


def call(body, outs, *args, scalars=None, mib=24):
    vm = pl.BlockSpec(memory_space=pltpu.VMEM)
    sm = pl.BlockSpec(memory_space=pltpu.SMEM)
    ins = ([sm] if scalars is not None else []) + [vm] * len(args)
    if scalars is not None:
        args = (scalars,) + tuple(args)
    return pl.pallas_call(
        body,
        out_shape=outs,
        in_specs=ins,
        out_specs=jax.tree.map(lambda _: vm, outs),
        compiler_params=pltpu.CompilerParams(vmem_limit_bytes=mib << 20),
    )(*args)


def hbm(x):
    return pltpu.with_memory_space_constraint(x, pltpu.HBM)


def swap(x, axis, m):
    n = lax.axis_size(axis)
    return lax.ppermute(x, axis, [(i, i ^ m) for i in range(n)])


def wide(t, width):
    return pl.ds(pl.multiple_of(t * width, width), width)


def landing(groups, cap, s, routes_ref):
    tok = routes_ref.shape[1]
    e0, e1 = routes_ref[0:1, :], routes_ref[1:2, :]
    ids = lax.broadcasted_iota(jnp.int32, (groups, tok), 0)
    hit0, hit1 = ids == e0, ids == e1
    member = jnp.where(hit0 | hit1, 1.0, 0.0).astype(BF16)
    upper = (
        lax.broadcasted_iota(jnp.int32, (tok, tok), 0)
        < lax.broadcasted_iota(jnp.int32, (tok, tok), 1)
    )
    rank = dot(member, jnp.where(upper, 1.0, 0.0).astype(BF16))
    r0 = jnp.sum(jnp.where(hit0, rank, 0.0), axis=0, keepdims=True).astype(jnp.int32)
    r1 = jnp.sum(jnp.where(hit1, rank, 0.0), axis=0, keepdims=True).astype(jnp.int32)
    return (e0 ^ s) * cap + r0, (e1 ^ s) * cap + r1


def picked(groups, cap, place_ref, routes_ref):
    land0, land1 = landing(groups, cap, place_ref[0], routes_ref)
    slots = lax.broadcasted_iota(jnp.int32, (groups * cap, routes_ref.shape[1]), 0)
    in0, in1 = slots == land0, slots == land1
    return in0, in1, jnp.where(in0 | in1, 1.0, 0.0).astype(BF16)


def scales(in0, in1, weight_ref):
    weight = jnp.where(in0, weight_ref[0:1, :], 0.0) + jnp.where(in1, weight_ref[1:2, :], 0.0)
    return jnp.sum(weight, axis=1, keepdims=True)


def far_body(groups, near, tps, cap, place_ref, routes_ref, weight_ref, normed_ref, cot_ref, *outs):
    count = groups - near
    xs, ys, whole = outs[:count], outs[count : 2 * count], outs[2 * count :]
    quarter = wide(place_ref[1], normed_ref.shape[1] // tps)
    in0, in1, pick = picked(groups, cap, place_ref, routes_ref)
    cut = near * cap
    x = dot(pick[cut:, :], normed_ref[:, quarter]).astype(BF16)
    y = dot(pick[cut:, :], cot_ref[:, quarter]) * scales(in0[cut:, :], in1[cut:, :], weight_ref)
    y = y.astype(BF16)
    for m in range(count):
        xs[m][...] = x[m * cap : (m + 1) * cap, :]
        ys[m][...] = y[m * cap : (m + 1) * cap, :]
    x = dot(pick[2 * cap : cut, :], normed_ref[...]).astype(BF16)
    for m, out in enumerate(whole):
        out[...] = x[m * cap : (m + 1) * cap, :]


def near_body(groups, near, cap, place_ref, routes_ref, weight_ref, normed_ref, cot_ref, edge_ref, *outs):
    in0, in1, pick = picked(groups, cap, place_ref, routes_ref)
    cut = near * cap
    edge = edge_ref[...]
    x = dot(pick[: 2 * cap, :], normed_ref[...]).astype(BF16)
    y = dot(pick[:cut, :], cot_ref[...]) * scales(in0[:cut, :], in1[:cut, :], weight_ref)
    y = y.astype(BF16)
    for m, out in enumerate(outs):
        out[:cap, :] = y[m * cap : (m + 1) * cap, :]
        out[cap : cap + 8, :] = jnp.zeros((8, out.shape[1]), BF16)
        out[cap : cap + 8, : edge.shape[1]] = edge
        if m < 2:
            out[cap + 8 :, :] = x[m * cap : (m + 1) * cap, :]


def edges_body(cap, *refs):
    out_ref = refs[-1]
    for m, r in enumerate(refs[:-1]):
        out_ref[8 * m : 8 * m + 8, :] = r[cap : cap + 8, : out_ref.shape[1]]


def join_body(cap, *refs):
    for m, r in enumerate(refs[:-1]):
        refs[-1][m * cap : (m + 1) * cap, :] = r[:cap, :]


def column(row):
    n = row.shape[1]
    eye = (
        lax.broadcasted_iota(jnp.int32, (n, n), 0)
        == lax.broadcasted_iota(jnp.int32, (n, n), 1)
    )
    return jnp.sum(jnp.where(eye, row, 0.0), axis=1, keepdims=True)


def slots_body(groups, cap, place_ref, routes_ref, out_ref):
    land0, land1 = landing(groups, cap, place_ref[0], routes_ref)
    land0 = column(land0.astype(F32)).astype(jnp.int32)
    land1 = column(land1.astype(F32)).astype(jnp.int32)
    slots = lax.broadcasted_iota(jnp.int32, out_ref.shape, 1)
    out_ref[...] = jnp.where((slots == land0) | (slots == land1), 1.0, 0.0).astype(BF16)


def shifted(x, by, fill, down):
    pad = jnp.full((by, x.shape[1]), fill, x.dtype)
    return (
        jnp.concatenate([pad, x[:-by, :]], axis=0)
        if down
        else jnp.concatenate([x[by:, :], pad], axis=0)
    )


def scan(keep, value, forward):
    by = 1
    while by < keep.shape[0]:
        value = keep * shifted(value, by, 0.0, forward) + value
        keep = keep * shifted(keep, by, 1.0, forward)
        by *= 2
    return keep, value


def forward_body(keep_ref, driven_ref, cum_ref, state_ref, tail_ref, edge_ref):
    keep = keep_ref[...]
    cum, state = scan(keep, driven_ref[...], True)
    tail = shifted(keep, 1, 1.0, False)
    by = 1
    while by < keep.shape[0]:
        tail = tail * shifted(tail, by, 1.0, False)
        by *= 2
    cum_ref[...] = cum
    state_ref[...] = state
    tail_ref[...] = tail
    edge = [cum[-1:, :], state[-1:, :], keep[:1, :] * tail[:1, :]]
    edge_ref[...] = jnp.concatenate(pair_of(edge), axis=0).astype(BF16)


def pair_of(rows):
    high = [r.astype(BF16).astype(F32) for r in rows]
    both = high + [r - h for r, h in zip(rows, high)]
    return both + [jnp.zeros_like(rows[0])] * (8 - len(both))


def enter_body(groups, place_ref, cum_ref, state_ref, k1_ref, k2_ref, edges_ref, hidden_ref, kk_ref, coef_ref):
    s = place_ref[0]
    chan = cum_ref.shape[1]
    edges = []
    for m in range(groups):
        e = edges_ref[8 * m : 8 * m + 8, :].astype(F32)
        edges.append(e[:3, :] + e[3:6, :])

    def edge(i, row):
        out = edges[0][row : row + 1, :]
        for m in range(1, groups):
            out = jnp.where((s ^ m) == i, edges[m][row : row + 1, :], out)
        return out

    state_in = jnp.zeros((1, chan), F32)
    product = jnp.ones((1, chan), F32)
    coefs = []
    for i in range(groups):
        state_in = jnp.where(i < s, state_in * edge(i, 0) + edge(i, 1), state_in)
        coefs.append(jnp.where(i > s, product, 0.0))
        product = jnp.where(i > s, product * edge(i, 2), product)
    state = state_ref[...] + cum_ref[...] * state_in
    hidden_ref[...] = state.astype(BF16)
    before = jnp.concatenate([state_in, state[:-1, :]], axis=0)
    kk_ref[...] = before * k1_ref[...] + k2_ref[...]
    for m in range(groups):
        out = jnp.zeros((1, chan), F32)
        for i in range(groups):
            out = jnp.where((s ^ m) == i, coefs[i], out)
        coef_ref[m : m + 1, :] = out


def put(out_ref, first, t, tps, pieces):
    for i, piece in enumerate(pieces):
        rows, width = piece.shape
        out_ref[first : first + rows, wide(t ^ (i % tps), width)] = piece[...]
        if i % tps == tps - 1:
            first += rows


def hidden_body(near, tps, cap, place_ref, gate_ref, up_ref, *rest):
    refs, (act_ref, swish_ref, slope_ref, x_ref) = rest[:-4], rest[-4:]
    for m in range(near):
        first = cap + 8 if m < 2 else 0
        x_ref[m * cap : (m + 1) * cap, :] = refs[m][first : first + cap, :]
    put(x_ref, near * cap, place_ref[1], tps, refs[near:])
    x = x_ref[...]
    gate = dot(x, gate_ref[...])
    up = dot(x, up_ref[...])
    sigma = jax.nn.sigmoid(gate)
    swish = gate * sigma
    act_ref[...] = (swish * up).astype(BF16)
    swish_ref[...] = swish
    slope_ref[...] = up * sigma * (1.0 + gate * (1.0 - sigma))


def back_body(first, near, tps, cap, place_ref, gate_ref, up_ref, down_ref, swish_ref, slope_ref, *rest):
    count = len(rest) - 3 - tps
    refs, (y_ref, dg_ref, du_ref, *outs) = rest[:count], rest[count:]
    t = place_ref[1]
    if near:
        for m in range(near):
            y_ref[m * cap : (m + 1) * cap, :] = refs[m][:cap, :]
    else:
        put(y_ref, 0, t, tps, refs)
    rows = y_ref.shape[0]
    at = slice(first, first + rows)
    d_act = dot(y_ref[...], down_ref[...], COLS)
    dg = (d_act * slope_ref[at, :]).astype(BF16)
    du = (d_act * swish_ref[at, :]).astype(BF16)
    dg_ref[...] = dg
    du_ref[...] = du
    width = gate_ref.shape[0] // tps

    def part(j):
        cols = wide(t ^ j, width)
        return dot(dg, gate_ref[cols, :], COLS) + dot(du, up_ref[cols, :], COLS)

    if tps != 4:
        for j in range(tps):
            outs[j][...] = part(j).astype(BF16)
        return
    half = rows // 2
    send_a, send_b, keep_a, keep_b = outs
    last = part(3).astype(BF16)
    send_a[half:, :] = last[:half, :]
    send_b[half:, :] = last[half:, :]
    one = part(1)
    send_a[:half, :] = one[:half, :].astype(BF16)
    keep_b[half:, :] = one[half:, :]
    two = part(2)
    send_b[:half, :] = two[half:, :].astype(BF16)
    keep_a[half:, :] = two[:half, :]
    mine = part(0)
    keep_a[:half, :] = mine[:half, :]
    keep_b[:half, :] = mine[half:, :]


def middle_body(keep_a, keep_b, got_a, got_b, stay_a, stay_b, go_a, go_b):
    half = stay_a.shape[0]
    for keep, got, stay, go in ((keep_a, got_a, stay_a, go_a), (keep_b, got_b, stay_b, go_b)):
        stay[...] = keep[:half, :] + got[:half, :].astype(F32)
        go[...] = (keep[half:, :] + got[half:, :].astype(F32)).astype(BF16)


def last_body(cap, stay_a, stay_b, got_a, got_b, *outs):
    half = len(outs) // 2
    a = (stay_a[...] + got_a[...].astype(F32)).astype(BF16)
    b = (stay_b[...] + got_b[...].astype(F32)).astype(BF16)
    for m, o in enumerate(outs):
        i = m % half
        o[...] = (a if m < half else b)[i * cap : (i + 1) * cap, :]


def grads_body(split, act_ref, x_ref, dg0_ref, du0_ref, y0_ref, dg1_ref, du1_ref, y1_ref, gg_ref, gu_ref, gd_ref):
    x0, x1 = x_ref[:split, :], x_ref[split:, :]
    gg_ref[...] = (dot(x0, dg0_ref[...], ROWS) + dot(x1, dg1_ref[...], ROWS)).astype(BF16)
    gu_ref[...] = (dot(x0, du0_ref[...], ROWS) + dot(x1, du1_ref[...], ROWS)).astype(BF16)
    a0, a1 = act_ref[:split, :], act_ref[split:, :]
    gd_ref[...] = (dot(a0, y0_ref[...], ROWS) + dot(a1, y1_ref[...], ROWS)).astype(BF16)


def sums_body(cap, *refs):
    count = refs[0].shape[0] // cap
    pieces, outs = refs[:-count], refs[-count:]
    total = pieces[0][...].astype(F32)
    for p in pieces[1:]:
        total = total + p[...].astype(F32)
    for m, o in enumerate(outs):
        o[...] = total[m * cap : (m + 1) * cap, :].astype(BF16)


def combine_body(slots_ref, *rest):
    blocks, out_ref = rest[:-1], rest[-1]
    rows = jnp.concatenate([b[...] for b in blocks], axis=0)
    out_ref[...] = dot(slots_ref[...], rows).astype(BF16)


def mix_body(tps, place_ref, inv_ref, gain_ref, normed_ref, cot_ref, mat_ref, keep_ref, *rest):
    pieces, (grad_ref, *strips, dn_ref, mix_ref) = rest[:tps], rest[tps:]
    s, t = place_ref[0], place_ref[1]
    for j in range(tps):
        dn_ref[:, wide(t ^ j, pieces[j].shape[1])] = pieces[j][...]
    dn = dn_ref[...].astype(F32)
    normed = normed_ref[...].astype(F32)
    gain = gain_ref[...]
    stat = jnp.sum(dn * normed, axis=1, keepdims=True) * (1.0 / dn.shape[1])
    mix = cot_ref[...].astype(F32) + column(inv_ref[...]) * (gain * dn - (normed / gain) * stat)
    mix = mix.astype(BF16)
    mix_ref[...] = mix
    keep = keep_ref[...]
    d_state = dot(mix, mat_ref[...])
    _, grad = scan(shifted(keep, 1, 1.0, False), d_state, False)
    grad_ref[...] = grad
    late = jnp.concatenate(pair_of([keep[:1, :] * grad[:1, :]]), axis=0).astype(BF16)
    tok, chan = keep.shape
    width = strips[0].shape[1]
    for m, out in enumerate(strips):
        if width % 128:
            both = mix_ref[:, wide((s ^ m) // 2, 2 * width)].astype(F32)
            odd = ((s ^ m) & 1) == 1
            out[:tok, :] = jnp.where(odd, both[:, width:], both[:, :width]).astype(BF16)
        else:
            out[:tok, :] = mix_ref[:, wide(s ^ m, width)]
        out[tok:, :] = jnp.zeros((8, width), BF16)
        out[tok:, :chan] = late


def final_body(groups, tok, coef_ref, grad_ref, tail_ref, opened_ref, kk_ref, slope_ref, hid_even_ref, hid_odd_ref, *rest):
    strips, (out_ref, rec_ref, decay_ref, gate_ref) = rest[:groups], rest[groups:]
    chan = grad_ref.shape[1]
    enter = jnp.zeros((1, chan), F32)
    weight = jnp.zeros(out_ref.shape, F32)
    for m in range(groups):
        hidden = (hid_odd_ref if m % 2 else hid_even_ref)[m // 2 * tok : (m // 2 + 1) * tok, :]
        late = strips[m][tok : tok + 8, :chan].astype(F32)
        enter = enter + coef_ref[m : m + 1, :] * (late[0:1, :] + late[1:2, :])
        weight = weight + dot(strips[m][:tok, :], hidden, ROWS)
    out_ref[...] = weight
    total = grad_ref[...] + tail_ref[...] * enter
    rec_ref[...] = total * opened_ref[...]
    decay_ref[...] = total * kk_ref[...]
    gate_ref[...] = total * slope_ref[...]


def sds(shape, dtype):
    return jax.ShapeDtypeStruct(shape, dtype)


def shards(
    cotangent,
    normed,
    inverse_root_mean_square,
    expert_norm_scale,
    routes,
    route_probability_weight,
    gate_weight,
    up_weight,
    down_weight,
    recurrence_input,
    recurrence_gate_logits,
    input_gate_logits,
    channel_decay_weight,
    extra_log_decay,
    output_matrix,
):
    tok, features = normed.shape
    groups, tps = lax.axis_size("sp"), lax.axis_size("tp")
    cap = 2 * routes.shape[1] * tok // groups
    rows = groups * cap
    width = features // tps
    s, t = lax.axis_index("sp"), lax.axis_index("tp")
    place = jnp.stack([s, t]).astype(jnp.int32)
    gate_w, up_w, down_w = gate_weight[0], up_weight[0], down_weight[0]
    hid = gate_w.shape[1]
    chan = output_matrix.shape[1]

    near = min(4, groups)
    routes_t, weights_t = routes.T, route_probability_weight.T
    plane = sds((tok, chan), F32)
    thin = sds((tok, chan), BF16)

    far = groups - near
    block = sds((cap, width), BF16)
    packed = call(
        functools.partial(far_body, groups, near, tps, cap),
        [block] * (2 * far) + [sds((cap, features), BF16)] * (near - 2),
        hbm(routes_t),
        hbm(weights_t),
        hbm(normed),
        hbm(cotangent),
        scalars=place,
    )
    packed, recurrence_input, recurrence_gate_logits, input_gate_logits, extra_log_decay, channel_decay_weight = (
        lax.optimization_barrier(
            (packed, recurrence_input, recurrence_gate_logits, input_gate_logits, extra_log_decay, channel_decay_weight)
        )
    )
    xs = [swap(x, "sp", near + m) for m, x in enumerate(packed[:far])]
    ys = [swap(y, "sp", near + m) for m, y in enumerate(packed[far : 2 * far])]
    close_x = [swap(x, "sp", 2 + m) for m, x in enumerate(packed[2 * far :])]

    retain = jax.nn.sigmoid(recurrence_gate_logits.astype(F32))
    admit = jax.nn.sigmoid(input_gate_logits.astype(F32))
    signal = recurrence_input.astype(F32)
    speed = -8.0 * jax.nn.softplus(-channel_decay_weight)[None, :]
    log_keep = retain * speed + extra_log_decay
    keep = jnp.exp(log_keep)
    scale_in = jnp.sqrt(-jnp.expm1(2.0 * log_keep))
    opened = scale_in * admit
    driven = opened * signal
    slope = driven * (1.0 - admit)
    decay = speed * retain * (1.0 - retain)
    k1 = keep * decay
    k2 = -admit * signal * keep * keep / scale_in * decay
    cum, state_loc, tail, edge = call(
        forward_body, [plane, plane, plane, sds((8, chan), BF16)], keep, driven
    )

    close_y = call(
        functools.partial(near_body, groups, near, cap),
        [sds(((cap if m > 1 else 2 * cap) + 8, features), BF16) for m in range(near)],
        hbm(routes_t),
        hbm(weights_t),
        hbm(normed),
        hbm(cotangent),
        edge,
        scalars=place,
    )
    close_y = [close_y[0]] + [swap(c, "sp", m) for m, c in enumerate(close_y) if m]
    edges = call(functools.partial(edges_body, cap), sds((8 * near, chan), BF16), *close_y)
    step = near
    while step < groups:
        edges = jnp.concatenate([edges, swap(edges, "sp", step)], axis=0)
        step *= 2

    def spread(blocks):
        mine = call(
            functools.partial(join_body, cap), sds((len(blocks) * cap, width), BF16), *blocks
        )
        return [mine] + [swap(mine, "tp", j) for j in range(1, tps)]

    xp = spread(xs)
    half = far // 2
    yp = spread(ys[:half]) + spread(ys[half:])

    hidden, kk, coef = call(
        functools.partial(enter_body, groups),
        [thin, plane, sds((groups, chan), F32)],
        cum,
        state_loc,
        k1,
        k2,
        edges,
        scalars=place,
    )
    slots = call(
        functools.partial(slots_body, groups, cap), sds((tok, rows), BF16), routes_t, scalars=place
    )

    wide_rows = sds((rows, hid), F32)
    thin_rows = sds((rows, hid), BF16)
    full_rows = sds((rows, features), BF16)
    act, swish, bend, x_all = call(
        functools.partial(hidden_body, near, tps, cap),
        [thin_rows, wide_rows, wide_rows, full_rows],
        gate_w,
        up_w,
        *close_y[:2],
        *close_x,
        *xp,
        scalars=place,
    )

    def back(first, count, refs):
        n = count * cap
        piece = sds((n, width), BF16)
        keep_rows = sds((n, width), F32)
        return call(
            functools.partial(back_body, first, 0 if first else near, tps, cap),
            [sds((n, features), BF16), sds((n, hid), BF16), sds((n, hid), BF16)]
            + ([piece, piece, keep_rows, keep_rows] if tps == 4 else [piece] * tps),
            gate_w,
            up_w,
            down_w,
            swish,
            bend,
            *refs,
            scalars=place,
        )

    y1, dg1, du1, *parts1 = back(near * cap, far, yp)
    y0, dg0, du0, *parts0 = back(0, near, close_y)
    grads = call(
        functools.partial(grads_body, near * cap),
        [sds((features, hid), BF16), sds((features, hid), BF16), sds((hid, features), BF16)],
        act,
        x_all,
        dg0,
        du0,
        y0,
        dg1,
        du1,
        y1,
    )

    def reduced(parts, count):
        outs = [block] * count
        if tps != 4:
            got = [parts[0]] + [swap(parts[j], "tp", j) for j in range(1, tps)]
            return call(functools.partial(sums_body, cap), outs, *got)
        send_a, send_b, keep_a, keep_b = parts
        got_a, got_b = swap(send_a, "tp", 1), swap(send_b, "tp", 2)
        n = count * cap // 2
        stay_a, stay_b, go_a, go_b = call(
            middle_body,
            [sds((n, width), F32)] * 2 + [sds((n, width), BF16)] * 2,
            keep_a,
            keep_b,
            got_a,
            got_b,
        )
        got_a, got_b = swap(go_a, "tp", 2), swap(go_b, "tp", 1)
        return call(functools.partial(last_body, cap), outs, stay_a, stay_b, got_a, got_b)

    summed = reduced(parts1, far)
    summed = list(reduced(parts0, near)) + list(summed)
    blocks = [summed[0]] + [swap(b, "sp", m) for m, b in enumerate(summed) if m]
    grad_gate, grad_up, grad_down = grads
    hid_even = jnp.concatenate(
        [hidden] + [swap(hidden, "sp", m) for m in range(2, groups, 2)], axis=0
    )
    hid_odd = swap(hid_even, "sp", 1)

    d_norm = call(combine_body, sds((tok, width), BF16), slots, *blocks)
    norms = [d_norm] + [swap(d_norm, "tp", j) for j in range(1, tps)]
    strip = features // groups
    grad_loc, *strips = call(
        functools.partial(mix_body, tps),
        [plane] + [sds((tok + 8, strip), BF16)] * groups + [sds((tok, features), BF16)] * 2,
        inverse_root_mean_square[None, :],
        expert_norm_scale[None, :],
        normed,
        cotangent,
        output_matrix,
        keep,
        *norms,
        scalars=place,
    )[:-2]
    strips = [strips[0]] + [swap(c, "sp", m) for m, c in enumerate(strips) if m]
    grad_out_weight, grad_rec, grad_decay, grad_input = call(
        functools.partial(final_body, groups, tok),
        [sds((strip, chan), F32), plane, plane, plane],
        coef,
        grad_loc,
        tail,
        opened,
        kk,
        slope,
        hid_even,
        hid_odd,
        *strips,
    )
    return (
        grad_gate[None],
        grad_up[None],
        grad_down[None],
        grad_out_weight,
        grad_rec,
        grad_decay,
        grad_input,
    )


def solution(mesh):
    return jax.shard_map(
        shards,
        mesh=mesh,
        in_specs=(
            P("sp", None),
            P("sp", None),
            P("sp"),
            P(),
            P("sp", None),
            P("sp", None),
            P("sp", None, "tp"),
            P("sp", None, "tp"),
            P("sp", "tp", None),
            P("sp", "tp"),
            P("sp", "tp"),
            P("sp", "tp"),
            P("tp"),
            P("sp", "tp"),
            P(None, "tp"),
        ),
        out_specs=(
            P("sp", None, "tp"),
            P("sp", None, "tp"),
            P("sp", "tp", None),
            P("sp", "tp"),
            P("sp", "tp"),
            P("sp", "tp"),
            P("sp", "tp"),
        ),
        check_vma=False,
    )
```

```python
import functools

import jax
import jax.numpy as jnp
from jax import lax
from jax.experimental import pallas as pl
from jax.experimental.pallas import tpu as pltpu
from jax.sharding import PartitionSpec as P


F32, BF16 = jnp.float32, jnp.bfloat16
ROWS = (((0,), (0,)), ((), ()))
COLS = (((1,), (1,)), ((), ()))
PLAIN = (((1,), (0,)), ((), ()))


def dot(a, b, dims=PLAIN):
    return lax.dot_general(a, b, dims, preferred_element_type=F32)


def call(body, outs, *args, scalars=None, mib=24, scratch=()):
    vm = pl.BlockSpec(memory_space=pltpu.VMEM)
    sm = pl.BlockSpec(memory_space=pltpu.SMEM)
    ins = ([sm] if scalars is not None else []) + [vm] * len(args)
    if scalars is not None:
        args = (scalars,) + tuple(args)
    return pl.pallas_call(
        body,
        out_shape=outs,
        in_specs=ins,
        out_specs=jax.tree.map(lambda _: vm, outs),
        scratch_shapes=[pltpu.VMEM(x.shape, x.dtype) for x in scratch],
        compiler_params=pltpu.CompilerParams(vmem_limit_bytes=mib << 20),
    )(*args)


def hbm(x):
    return pltpu.with_memory_space_constraint(x, pltpu.HBM)


def swap(x, axis, m):
    n = lax.axis_size(axis)
    return lax.ppermute(x, axis, [(i, i ^ m) for i in range(n)])


def wide(t, width):
    return pl.ds(pl.multiple_of(t * width, width), width)


def landing(groups, cap, s, routes_ref):
    tok = routes_ref.shape[1]
    e0, e1 = routes_ref[0:1, :], routes_ref[1:2, :]
    ids = lax.broadcasted_iota(jnp.int32, (groups, tok), 0)
    hit0, hit1 = ids == e0, ids == e1
    member = jnp.where(hit0 | hit1, 1.0, 0.0).astype(BF16)
    upper = (
        lax.broadcasted_iota(jnp.int32, (tok, tok), 0)
        < lax.broadcasted_iota(jnp.int32, (tok, tok), 1)
    )
    rank = dot(member, jnp.where(upper, 1.0, 0.0).astype(BF16))
    r0 = jnp.sum(jnp.where(hit0, rank, 0.0), axis=0, keepdims=True).astype(jnp.int32)
    r1 = jnp.sum(jnp.where(hit1, rank, 0.0), axis=0, keepdims=True).astype(jnp.int32)
    return (e0 ^ s) * cap + r0, (e1 ^ s) * cap + r1


def picked(groups, cap, place_ref, routes_ref):
    land0, land1 = landing(groups, cap, place_ref[0], routes_ref)
    slots = lax.broadcasted_iota(jnp.int32, (groups * cap, routes_ref.shape[1]), 0)
    in0, in1 = slots == land0, slots == land1
    return in0, in1, jnp.where(in0 | in1, 1.0, 0.0).astype(BF16)


def scales(in0, in1, weight_ref):
    weight = jnp.where(in0, weight_ref[0:1, :], 0.0) + jnp.where(in1, weight_ref[1:2, :], 0.0)
    return jnp.sum(weight, axis=1, keepdims=True)


def far_body(groups, near, tps, cap, place_ref, routes_ref, weight_ref, normed_ref, cot_ref, *outs):
    count = groups - near
    xs, ys, whole = outs[:count], outs[count : 2 * count], outs[2 * count :]
    quarter = wide(place_ref[1], normed_ref.shape[1] // tps)
    in0, in1, pick = picked(groups, cap, place_ref, routes_ref)
    cut = near * cap
    x = dot(pick[cut:, :], normed_ref[:, quarter]).astype(BF16)
    y = dot(pick[cut:, :], cot_ref[:, quarter]) * scales(in0[cut:, :], in1[cut:, :], weight_ref)
    y = y.astype(BF16)
    for m in range(count):
        xs[m][...] = x[m * cap : (m + 1) * cap, :]
        ys[m][...] = y[m * cap : (m + 1) * cap, :]
    x = dot(pick[2 * cap : cut, :], normed_ref[...]).astype(BF16)
    for m, out in enumerate(whole):
        out[...] = x[m * cap : (m + 1) * cap, :]


def near_body(groups, near, cap, place_ref, routes_ref, weight_ref, normed_ref, cot_ref, edge_ref, *outs):
    in0, in1, pick = picked(groups, cap, place_ref, routes_ref)
    cut = near * cap
    edge = edge_ref[...]
    x = dot(pick[: 2 * cap, :], normed_ref[...]).astype(BF16)
    y = dot(pick[:cut, :], cot_ref[...]) * scales(in0[:cut, :], in1[:cut, :], weight_ref)
    y = y.astype(BF16)
    for m, out in enumerate(outs):
        out[:cap, :] = y[m * cap : (m + 1) * cap, :]
        out[cap : cap + 8, :] = jnp.zeros((8, out.shape[1]), BF16)
        out[cap : cap + 8, : edge.shape[1]] = edge
        if m < 2:
            out[cap + 8 :, :] = x[m * cap : (m + 1) * cap, :]


def edges_body(cap, *refs):
    out_ref = refs[-1]
    for m, r in enumerate(refs[:-1]):
        out_ref[8 * m : 8 * m + 8, :] = r[cap : cap + 8, : out_ref.shape[1]]


def join_body(cap, *refs):
    for m, r in enumerate(refs[:-1]):
        refs[-1][m * cap : (m + 1) * cap, :] = r[:cap, :]


def column(row):
    n = row.shape[1]
    eye = (
        lax.broadcasted_iota(jnp.int32, (n, n), 0)
        == lax.broadcasted_iota(jnp.int32, (n, n), 1)
    )
    return jnp.sum(jnp.where(eye, row, 0.0), axis=1, keepdims=True)


def slots_body(groups, cap, place_ref, routes_ref, out_ref):
    land0, land1 = landing(groups, cap, place_ref[0], routes_ref)
    land0 = column(land0.astype(F32)).astype(jnp.int32)
    land1 = column(land1.astype(F32)).astype(jnp.int32)
    slots = lax.broadcasted_iota(jnp.int32, out_ref.shape, 1)
    out_ref[...] = jnp.where((slots == land0) | (slots == land1), 1.0, 0.0).astype(BF16)


def shifted(x, by, fill, down):
    pad = jnp.full((by, x.shape[1]), fill, x.dtype)
    return (
        jnp.concatenate([pad, x[:-by, :]], axis=0)
        if down
        else jnp.concatenate([x[by:, :], pad], axis=0)
    )


def scan(keep, value, forward):
    by = 1
    while by < keep.shape[0]:
        value = keep * shifted(value, by, 0.0, forward) + value
        keep = keep * shifted(keep, by, 1.0, forward)
        by *= 2
    return keep, value


def forward_body(keep_ref, driven_ref, cum_ref, state_ref, tail_ref, edge_ref):
    keep = keep_ref[...]
    cum, state = scan(keep, driven_ref[...], True)
    tail = shifted(keep, 1, 1.0, False)
    by = 1
    while by < keep.shape[0]:
        tail = tail * shifted(tail, by, 1.0, False)
        by *= 2
    cum_ref[...] = cum
    state_ref[...] = state
    tail_ref[...] = tail
    edge = [cum[-1:, :], state[-1:, :], keep[:1, :] * tail[:1, :]]
    edge_ref[...] = jnp.concatenate(pair_of(edge), axis=0).astype(BF16)


def pair_of(rows):
    high = [r.astype(BF16).astype(F32) for r in rows]
    both = high + [r - h for r, h in zip(rows, high)]
    return both + [jnp.zeros_like(rows[0])] * (8 - len(both))


def enter_body(groups, place_ref, cum_ref, state_ref, k1_ref, k2_ref, edges_ref, hidden_ref, kk_ref, coef_ref):
    s = place_ref[0]
    chan = cum_ref.shape[1]
    edges = []
    for m in range(groups):
        e = edges_ref[8 * m : 8 * m + 8, :].astype(F32)
        edges.append(e[:3, :] + e[3:6, :])

    def edge(i, row):
        out = edges[0][row : row + 1, :]
        for m in range(1, groups):
            out = jnp.where((s ^ m) == i, edges[m][row : row + 1, :], out)
        return out

    state_in = jnp.zeros((1, chan), F32)
    product = jnp.ones((1, chan), F32)
    coefs = []
    for i in range(groups):
        state_in = jnp.where(i < s, state_in * edge(i, 0) + edge(i, 1), state_in)
        coefs.append(jnp.where(i > s, product, 0.0))
        product = jnp.where(i > s, product * edge(i, 2), product)
    state = state_ref[...] + cum_ref[...] * state_in
    hidden_ref[...] = state.astype(BF16)
    before = jnp.concatenate([state_in, state[:-1, :]], axis=0)
    kk_ref[...] = before * k1_ref[...] + k2_ref[...]
    for m in range(groups):
        out = jnp.zeros((1, chan), F32)
        for i in range(groups):
            out = jnp.where((s ^ m) == i, coefs[i], out)
        coef_ref[m : m + 1, :] = out


def put(out_ref, t, at, pieces):
    for (first, j), piece in zip(at, pieces):
        rows, width = piece.shape
        out_ref[first : first + rows, wide(t ^ j, width)] = piece[...]


def hidden_body(near, cap, at, place_ref, gate_ref, up_ref, *rest):
    refs, (act_ref, swish_ref, slope_ref, x_ref) = rest[:-4], rest[-4:]
    for m in range(near):
        first = cap + 8 if m < 2 else 0
        x_ref[m * cap : (m + 1) * cap, :] = refs[m][first : first + cap, :]
    put(x_ref, place_ref[1], at, refs[near:])
    x = x_ref[...]
    gate = dot(x, gate_ref[...])
    up = dot(x, up_ref[...])
    sigma = jax.nn.sigmoid(gate)
    swish = gate * sigma
    act_ref[...] = (swish * up).astype(BF16)
    swish_ref[...] = swish
    slope_ref[...] = up * sigma * (1.0 + gate * (1.0 - sigma))


def back_body(first, near, tps, cap, at, place_ref, gate_ref, up_ref, down_ref, swish_ref, slope_ref, *rest):
    count = len(rest) - 3 - tps
    refs, (y_ref, dg_ref, du_ref, *outs) = rest[:count], rest[count:]
    t = place_ref[1]
    if near:
        for m in range(near):
            y_ref[m * cap : (m + 1) * cap, :] = refs[m][:cap, :]
    else:
        put(y_ref, t, at, refs)
    rows = y_ref.shape[0]
    here = slice(first, first + rows)
    d_act = dot(y_ref[...], down_ref[...], COLS)
    dg = (d_act * slope_ref[here, :]).astype(BF16)
    du = (d_act * swish_ref[here, :]).astype(BF16)
    dg_ref[...] = dg
    du_ref[...] = du
    width = gate_ref.shape[0] // tps

    def part(j):
        cols = wide(t ^ j, width)
        return dot(dg, gate_ref[cols, :], COLS) + dot(du, up_ref[cols, :], COLS)

    if tps != 4:
        for j in range(tps):
            outs[j][...] = part(j).astype(BF16)
        return
    half = rows // 2
    send_a, send_b, keep_a, keep_b = outs
    last = part(3).astype(BF16)
    send_a[half:, :] = last[:half, :]
    send_b[half:, :] = last[half:, :]
    one = part(1)
    send_a[:half, :] = one[:half, :].astype(BF16)
    keep_b[half:, :] = one[half:, :]
    two = part(2)
    send_b[:half, :] = two[half:, :].astype(BF16)
    keep_a[half:, :] = two[:half, :]
    mine = part(0)
    keep_a[:half, :] = mine[:half, :]
    keep_b[:half, :] = mine[half:, :]


def middle_body(keep_a, keep_b, got_a, got_b, stay_a, stay_b, go_a, go_b):
    half = stay_a.shape[0]
    for keep, got, stay, go in ((keep_a, got_a, stay_a, go_a), (keep_b, got_b, stay_b, go_b)):
        stay[...] = keep[:half, :] + got[:half, :].astype(F32)
        go[...] = (keep[half:, :] + got[half:, :].astype(F32)).astype(BF16)


def last_body(cap, stay_a, stay_b, got_a, got_b, *outs):
    half = len(outs) // 2
    a = (stay_a[...] + got_a[...].astype(F32)).astype(BF16)
    b = (stay_b[...] + got_b[...].astype(F32)).astype(BF16)
    for m, o in enumerate(outs):
        i = m % half
        o[...] = (a if m < half else b)[i * cap : (i + 1) * cap, :]


def inner_body(split, x_ref, dg0_ref, du0_ref, dg1_ref, du1_ref, gg_ref, gu_ref):
    x0, x1 = x_ref[:split, :], x_ref[split:, :]
    gg_ref[...] = (dot(x0, dg0_ref[...], ROWS) + dot(x1, dg1_ref[...], ROWS)).astype(BF16)
    gu_ref[...] = (dot(x0, du0_ref[...], ROWS) + dot(x1, du1_ref[...], ROWS)).astype(BF16)


def outer_body(split, act_ref, y0_ref, y1_ref, gd_ref):
    a0, a1 = act_ref[:split, :], act_ref[split:, :]
    gd_ref[...] = (dot(a0, y0_ref[...], ROWS) + dot(a1, y1_ref[...], ROWS)).astype(BF16)


def sums_body(cap, *refs):
    count = refs[0].shape[0] // cap
    pieces, outs = refs[:-count], refs[-count:]
    total = pieces[0][...].astype(F32)
    for p in pieces[1:]:
        total = total + p[...].astype(F32)
    for m, o in enumerate(outs):
        o[...] = total[m * cap : (m + 1) * cap, :].astype(BF16)


def combine_body(slots_ref, *rest):
    blocks, out_ref = rest[:-1], rest[-1]
    rows = jnp.concatenate([b[...] for b in blocks], axis=0)
    out_ref[...] = dot(slots_ref[...], rows).astype(BF16)


def ratio_body(inv_ref, gain_ref, normed_ref, out_ref):
    out_ref[...] = column(inv_ref[...]) * normed_ref[...].astype(F32) / gain_ref[...]


def mix_body(tps, place_ref, inv_ref, gain_ref, ratio_ref, normed_ref, cot_ref, mat_ref, keep_ref, *rest):
    pieces, (grad_ref, *strips, dn_ref, mix_ref) = rest[:tps], rest[tps:]
    s, t = place_ref[0], place_ref[1]
    for j in range(tps):
        dn_ref[:, wide(t ^ j, pieces[j].shape[1])] = pieces[j][...]
    dn = dn_ref[...].astype(F32)
    normed = normed_ref[...].astype(F32)
    stat = jnp.sum(dn * normed, axis=1, keepdims=True) * (1.0 / dn.shape[1])
    mix = cot_ref[...].astype(F32) + (column(inv_ref[...]) * gain_ref[...]) * dn - ratio_ref[...] * stat
    mix = mix.astype(BF16)
    mix_ref[...] = mix
    keep = keep_ref[...]
    d_state = dot(mix, mat_ref[...])
    _, grad = scan(shifted(keep, 1, 1.0, False), d_state, False)
    grad_ref[...] = grad
    late = jnp.concatenate(pair_of([keep[:1, :] * grad[:1, :]]), axis=0).astype(BF16)
    tok, chan = keep.shape
    width = strips[0].shape[1]
    for m, out in enumerate(strips):
        if width % 128:
            both = mix_ref[:, wide((s ^ m) // 2, 2 * width)].astype(F32)
            odd = ((s ^ m) & 1) == 1
            out[:tok, :] = jnp.where(odd, both[:, width:], both[:, :width]).astype(BF16)
        else:
            out[:tok, :] = mix_ref[:, wide(s ^ m, width)]
        out[tok:, :] = jnp.zeros((8, width), BF16)
        out[tok:, :chan] = late


def final_body(groups, tok, coef_ref, grad_ref, tail_ref, opened_ref, kk_ref, slope_ref, hid_even_ref, hid_odd_ref, *rest):
    strips, (out_ref, rec_ref, decay_ref, gate_ref) = rest[:groups], rest[groups:]
    chan = grad_ref.shape[1]
    enter = jnp.zeros((1, chan), F32)
    weight = jnp.zeros(out_ref.shape, F32)
    for m in range(groups):
        hidden = (hid_odd_ref if m % 2 else hid_even_ref)[m // 2 * tok : (m // 2 + 1) * tok, :]
        late = strips[m][tok : tok + 8, :chan].astype(F32)
        enter = enter + coef_ref[m : m + 1, :] * (late[0:1, :] + late[1:2, :])
        weight = weight + dot(strips[m][:tok, :], hidden, ROWS)
    out_ref[...] = weight
    total = grad_ref[...] + tail_ref[...] * enter
    rec_ref[...] = total * opened_ref[...]
    decay_ref[...] = total * kk_ref[...]
    gate_ref[...] = total * slope_ref[...]


def sds(shape, dtype):
    return jax.ShapeDtypeStruct(shape, dtype)


def shards(
    cotangent,
    normed,
    inverse_root_mean_square,
    expert_norm_scale,
    routes,
    route_probability_weight,
    gate_weight,
    up_weight,
    down_weight,
    recurrence_input,
    recurrence_gate_logits,
    input_gate_logits,
    channel_decay_weight,
    extra_log_decay,
    output_matrix,
):
    tok, features = normed.shape
    groups, tps = lax.axis_size("sp"), lax.axis_size("tp")
    cap = 2 * routes.shape[1] * tok // groups
    rows = groups * cap
    width = features // tps
    s, t = lax.axis_index("sp"), lax.axis_index("tp")
    place = jnp.stack([s, t]).astype(jnp.int32)
    gate_w, up_w, down_w = gate_weight[0], up_weight[0], down_weight[0]
    hid = gate_w.shape[1]
    chan = output_matrix.shape[1]

    near = min(4, groups)
    routes_t, weights_t = routes.T, route_probability_weight.T
    plane = sds((tok, chan), F32)
    thin = sds((tok, chan), BF16)

    far = groups - near
    block = sds((cap, width), BF16)
    packed = call(
        functools.partial(far_body, groups, near, tps, cap),
        [block] * (2 * far) + [sds((cap, features), BF16)] * (near - 2),
        hbm(routes_t),
        hbm(weights_t),
        hbm(normed),
        hbm(cotangent),
        scalars=place,
    )
    packed, recurrence_input, recurrence_gate_logits, input_gate_logits, extra_log_decay, channel_decay_weight = (
        lax.optimization_barrier(
            (packed, recurrence_input, recurrence_gate_logits, input_gate_logits, extra_log_decay, channel_decay_weight)
        )
    )
    xs = [swap(x, "sp", near + m) for m, x in enumerate(packed[:far])]
    ys = [swap(y, "sp", near + m) for m, y in enumerate(packed[far : 2 * far])]
    close_x = [swap(x, "sp", 2 + m) for m, x in enumerate(packed[2 * far :])]

    retain = jax.nn.sigmoid(recurrence_gate_logits.astype(F32))
    admit = jax.nn.sigmoid(input_gate_logits.astype(F32))
    signal = recurrence_input.astype(F32)
    speed = -8.0 * jax.nn.softplus(-channel_decay_weight)[None, :]
    log_keep = retain * speed + extra_log_decay
    keep = jnp.exp(log_keep)
    scale_in = jnp.sqrt(-jnp.expm1(2.0 * log_keep))
    opened = scale_in * admit
    driven = opened * signal
    slope = driven * (1.0 - admit)
    decay = speed * retain * (1.0 - retain)
    k1 = keep * decay
    k2 = -admit * signal * keep * keep / scale_in * decay
    cum, state_loc, tail, edge = call(
        forward_body, [plane, plane, plane, sds((8, chan), BF16)], keep, driven
    )

    close_y = call(
        functools.partial(near_body, groups, near, cap),
        [sds(((cap if m > 1 else 2 * cap) + 8, features), BF16) for m in range(near)],
        hbm(routes_t),
        hbm(weights_t),
        hbm(normed),
        hbm(cotangent),
        edge,
        scalars=place,
    )
    close_y = [close_y[0]] + [swap(c, "sp", m) for m, c in enumerate(close_y) if m]
    edges = call(functools.partial(edges_body, cap), sds((8 * near, chan), BF16), *close_y)
    step = near
    while step < groups:
        edges = jnp.concatenate([edges, swap(edges, "sp", step)], axis=0)
        step *= 2

    def spread(blocks, first, direct):
        mine = call(
            functools.partial(join_body, cap), sds((len(blocks) * cap, width), BF16), *blocks
        )
        n = mine.shape[0]
        if tps != 4 or direct:
            pieces = [mine] + [swap(mine, "tp", j) for j in range(1, tps)]
            return pieces, [(first, j) for j in range(tps)]
        one, two = swap(mine, "tp", 1), swap(mine, "tp", 2)
        low = swap(one[: n // 2], "tp", 2)
        high = swap(two[n // 2 :], "tp", 1)
        return [mine, one, two, low, high], [
            (first, 0),
            (first, 1),
            (first, 2),
            (first, 3),
            (first + n // 2, 3),
        ]

    half = far // 2
    xp, at_x = spread(xs, near * cap, False)
    yp, at_y = spread(ys[:half], 0, True)
    wp, at_w = spread(ys[half:], half * cap, True)
    yp, at_y = yp + wp, at_y + at_w

    hidden, kk, coef = call(
        functools.partial(enter_body, groups),
        [thin, plane, sds((groups, chan), F32)],
        cum,
        state_loc,
        k1,
        k2,
        edges,
        scalars=place,
    )
    inverse, gains = inverse_root_mean_square[None, :], expert_norm_scale[None, :]
    ratio = call(ratio_body, sds((tok, features), F32), inverse, gains, normed)
    slots = call(
        functools.partial(slots_body, groups, cap), sds((tok, rows), BF16), routes_t, scalars=place
    )

    wide_rows = sds((rows, hid), F32)
    thin_rows = sds((rows, hid), BF16)
    full_rows = sds((rows, features), BF16)
    act, swish, bend, x_all = call(
        functools.partial(hidden_body, near, cap, at_x),
        [thin_rows, wide_rows, wide_rows, full_rows],
        gate_w,
        up_w,
        *close_y[:2],
        *close_x,
        *xp,
        scalars=place,
    )

    def back(first, count, refs):
        n = count * cap
        piece = sds((n, width), BF16)
        keep_rows = sds((n, width), F32)
        return call(
            functools.partial(back_body, first, 0 if first else near, tps, cap, at_y),
            [sds((n, features), BF16), sds((n, hid), BF16), sds((n, hid), BF16)]
            + ([piece, piece, keep_rows, keep_rows] if tps == 4 else [piece] * tps),
            gate_w,
            up_w,
            down_w,
            swish,
            bend,
            *refs,
            scalars=place,
        )

    y1, dg1, du1, *parts1 = back(near * cap, far, yp)
    y0, dg0, du0, *parts0 = back(0, near, close_y)
    grad_gate, grad_up = call(
        functools.partial(inner_body, near * cap),
        [sds((features, hid), BF16)] * 2,
        x_all,
        dg0,
        du0,
        dg1,
        du1,
    )
    grad_down = call(
        functools.partial(outer_body, near * cap), sds((hid, features), BF16), act, y0, y1
    )

    def reduced(parts, count):
        outs = [block] * count
        if tps != 4:
            got = [parts[0]] + [swap(parts[j], "tp", j) for j in range(1, tps)]
            return call(functools.partial(sums_body, cap), outs, *got)
        send_a, send_b, keep_a, keep_b = parts
        got_a, got_b = swap(send_a, "tp", 1), swap(send_b, "tp", 2)
        n = count * cap // 2
        stay_a, stay_b, go_a, go_b = call(
            middle_body,
            [sds((n, width), F32)] * 2 + [sds((n, width), BF16)] * 2,
            keep_a,
            keep_b,
            got_a,
            got_b,
        )
        got_a, got_b = swap(go_a, "tp", 2), swap(go_b, "tp", 1)
        return call(functools.partial(last_body, cap), outs, stay_a, stay_b, got_a, got_b)

    summed = reduced(parts1, far)
    summed = list(reduced(parts0, near)) + list(summed)
    blocks = [summed[0]] + [swap(b, "sp", m) for m, b in enumerate(summed) if m]
    hid_even = call(
        functools.partial(join_body, tok),
        sds((groups // 2 * tok, chan), BF16),
        hidden,
        *[swap(hidden, "sp", m) for m in range(2, groups, 2)],
    )
    hid_odd = swap(hid_even, "sp", 1)

    d_norm = call(combine_body, sds((tok, width), BF16), slots, *blocks)
    norms = [d_norm] + [swap(d_norm, "tp", j) for j in range(1, tps)]
    strip = features // groups
    grad_loc, *strips = call(
        functools.partial(mix_body, tps),
        [plane] + [sds((tok + 8, strip), BF16)] * groups,
        inverse,
        gains,
        ratio,
        normed,
        cotangent,
        output_matrix,
        keep,
        *norms,
        scalars=place,
        scratch=[sds((tok, features), BF16)] * 2,
    )
    strips = [strips[0]] + [swap(c, "sp", m) for m, c in enumerate(strips) if m]
    grad_out_weight, grad_rec, grad_decay, grad_input = call(
        functools.partial(final_body, groups, tok),
        [sds((strip, chan), F32), plane, plane, plane],
        coef,
        grad_loc,
        tail,
        opened,
        kk,
        slope,
        hid_even,
        hid_odd,
        *strips,
    )
    return (
        grad_gate[None],
        grad_up[None],
        grad_down[None],
        grad_out_weight,
        grad_rec,
        grad_decay,
        grad_input,
    )


def solution(mesh):
    return jax.shard_map(
        shards,
        mesh=mesh,
        in_specs=(
            P("sp", None),
            P("sp", None),
            P("sp"),
            P(),
            P("sp", None),
            P("sp", None),
            P("sp", None, "tp"),
            P("sp", None, "tp"),
            P("sp", "tp", None),
            P("sp", "tp"),
            P("sp", "tp"),
            P("sp", "tp"),
            P("tp"),
            P("sp", "tp"),
            P(None, "tp"),
        ),
        out_specs=(
            P("sp", None, "tp"),
            P("sp", None, "tp"),
            P("sp", "tp", None),
            P("sp", "tp"),
            P("sp", "tp"),
            P("sp", "tp"),
            P("sp", "tp"),
        ),
        check_vma=False,
    )
```
